512 devices in a mesh: ep: 32 (over z, core), tp: 16 (over y, x).
Axes of the slice: x: 4, y: 4, z: 16, core: 2. Of those that a mesh axis runs over, the one named last changes fastest.
Arguments:
- conv_input: bfloat16 [1024, 65536], P('tp', 'ep'), may hold values from -6 to 6
- out_gate: bfloat16 [1024, 65536], P('tp', 'ep'), may hold values from -6 to 6
- in_gate: bfloat16 [1024, 65536], P('tp', 'ep'), may hold values from -6 to 6
- conv_taps: float32 [3, 1024], replicated, may hold values from -3.5 to 3.5
- mixer_proj: bfloat16 [1024, 2048], P(None, 'tp'), may hold values from -0.1875 to 0.1875
- token_rows: bfloat16 [8192, 2048], P('ep', 'tp'), may hold values from -4000 to 4000
- routes: int32 [8192, 2], P('ep'), may hold values from 0 to 31, as said below
- route_weights: float32 [8192, 2], P('ep'), may hold values from 0.3 to 1
- expert_gate: bfloat16 [32, 2048, 4096], P('ep', None, 'tp'), may hold values from -0.125 to 0.125
- expert_up: bfloat16 [32, 2048, 4096], P('ep', None, 'tp'), may hold values from -0.125 to 0.125
- expert_down: bfloat16 [32, 4096, 2048], P('ep', 'tp'), may hold values from -0.125 to 0.125
Outputs:
- mixed_out: bfloat16 [65536, 2048], P('ep', 'tp')
- expert_out: bfloat16 [8192, 2048], P('ep', 'tp')
The draws below stay inside these ranges and needn't reach their ends.
Inputs may be any that keep to these rules, and one draw needn't show every extreme that they name: `routes`: in each aligned block of 256 rows, no expert is named more than 32 times and one expert, the same in every block, exactly 32 times; the two experts of a row differ.
All inputs are finite; a program needn't handle non-finite values.
Results may differ from the reference program's by a relative error of at most 0.015.
Values may be sent and summed in bfloat16 or wider, within the bound.
A program may use at most 64 MiB of HBM per device.

```python
import math
import jax
import jax.numpy as jnp
from jax import lax

D = 2048
W = 1024
FF = 4096
KERNEL = 3
ROWS_B = 256
EXPERTS = 32
FF_PART = 256
TOK_A = 65536
TOK_B = 8192
CAP = 32
N_TP = 16


def draw_token_rows(key, part):
    base_key, row_key, col_key = jax.random.split(key, 3)
    ramp = jnp.arange(D, dtype=jnp.float32) / D
    base = jnp.clip(jax.random.normal(base_key, (TOK_B, D), jnp.float32), -6.0, 6.0)
    row_scales = jnp.exp(jax.random.uniform(row_key, (TOK_B, 1), jnp.float32, 0.0, math.log(10.0)))
    col_scales = jnp.exp(math.log(10.0) * ramp) * jnp.exp(jax.random.uniform(col_key, (D,), jnp.float32, -0.4, 0.4))
    return (base * row_scales * col_scales[None, :]).astype(jnp.bfloat16)


def draw_routes(key, part):
    blocks = TOK_B // ROWS_B
    capacity = 4 * ROWS_B // EXPERTS
    spare = 2 * ROWS_B - capacity
    hottest = jax.random.randint(jax.random.fold_in(key, 7), (), 0, EXPERTS).astype(jnp.int32)
    ladder = jnp.arange(EXPERTS - 1, dtype=jnp.int32)
    weight_cum = (ladder + 1) * (ladder + 2) // 2
    weight_total = (EXPERTS - 1) * EXPERTS // 2
    run_ends = capacity + spare * weight_cum // weight_total
    position = jnp.arange(2 * ROWS_B, dtype=jnp.int32)
    which_run = jnp.sum((position[:, None] >= run_ends[None, :]).astype(jnp.int32), axis=1)
    which_run = jnp.minimum(which_run, EXPERTS - 2)

    def one_block(block_index):
        block_key = jax.random.fold_in(key, block_index + 11)
        order = jax.random.permutation(jax.random.fold_in(block_key, 1), EXPERTS - 1).astype(jnp.int32)
        others = (hottest + 1 + order) % EXPERTS
        listing = jnp.where(position < capacity, hottest, others[which_run])
        pairs = jnp.stack([listing[:ROWS_B], listing[ROWS_B:]], axis=1)
        shuffle = jax.random.permutation(jax.random.fold_in(block_key, 2), ROWS_B)
        return pairs[shuffle]
    table = jax.vmap(one_block)(jnp.arange(blocks, dtype=jnp.int32))
    return table.reshape(TOK_B, 2).astype(jnp.int32)


def spiked(drawn, rng, source, target, shards_of, factor):
    owner, partner = [(jnp.arange(drawn.shape[axis_at]) // (drawn.shape[axis_at] // shards_of)).reshape([-1 if axis == axis_at else 1 for axis in range(drawn.ndim)]) for axis_at in (source, target)]
    chosen = jax.random.permutation(rng, shards_of)[partner]
    strong = (owner == chosen) | (owner == (partner + shards_of // 2) % shards_of)
    return jnp.where(strong, factor * drawn, drawn)


def levels(rng, dims, shards, least, largest):
    def one(dim, blocks):
        heights = jax.random.uniform(jax.random.fold_in(jax.random.fold_in(rng, 6), dim), (blocks,), jnp.float32, least / len(shards), largest / len(shards))
        return jnp.repeat(jnp.exp(heights), dims[dim] // blocks).reshape((-1,) + (1,) * (len(dims) - dim - 1))

    factor_of = one(*shards[0])
    for cut in shards[1:]:
        factor_of = factor_of * one(*cut)
    return factor_of


def bell_draw(key, extent, scale, limit, pieces=(), kind=jnp.bfloat16):
    result = jax.random.normal(key, extent, jnp.float32) * scale
    if len(pieces) > 0:
        result = levels(key, extent, pieces, -0.22, 0.18) * result
    return jnp.clip(result, min=-limit, max=limit).astype(kind)


def noise_with(rng, shape, width, bound, cuts, heavy, held_as=jnp.bfloat16):
    drawn = width * jax.random.normal(rng, shape, jnp.float32)
    if cuts:
        drawn = drawn * levels(rng, shape, cuts, -0.22, 0.18)
    return jnp.clip(spiked(drawn, jax.random.fold_in(rng, 3), *heavy), -bound, bound).astype(held_as)


def setup_inputs(seed: int = 0) -> dict:
    seeds = jax.random.split(jax.random.key(seed), 12)
    return {
        "conv_input": bell_draw(seeds[0], (W, TOK_A), 1.0, 6.0, ((0, 16), (1, 32))),
        "out_gate": bell_draw(seeds[1], (W, TOK_A), 1.0, 6.0, ((0, 16), (1, 32))),
        "in_gate": bell_draw(seeds[2], (W, TOK_A), 1.0, 6.0, ((0, 16), (1, 32))),
        "conv_taps": bell_draw(seeds[3], (KERNEL, W), 0.6, 3.5, (), jnp.float32),
        "mixer_proj": bell_draw(seeds[4], (W, D), W ** -0.5, 0.1875, ((1, 16),)),
        "token_rows": draw_token_rows(jax.random.fold_in(seeds[11], 71), 0),
        "routes": draw_routes(jax.random.fold_in(seeds[11], 71), 0),
        "route_weights": jnp.clip(0.3 + 0.7 * jax.random.uniform(seeds[7], (TOK_B, 2), jnp.float32) ** levels(seeds[7], (TOK_B, 2), ((0, 32),), -0.2, 0.2), 0.3, 1.0),
        "expert_gate": bell_draw(seeds[8], (EXPERTS, D, FF), D ** -0.5, 0.125, ((0, 32), (2, 16))),
        "expert_up": bell_draw(seeds[9], (EXPERTS, D, FF), D ** -0.5, 0.125, ((0, 32), (2, 16))),
        "expert_down": noise_with(seeds[10], (EXPERTS, FF, D), FF ** -0.5, 0.125, ((0, 32), (1, 16)), (1, 2, 16, 2.0)),
    }


EPSILON = 1e-06

def slot_places(route_ids, capacity, experts):
    flat_ids = route_ids.reshape(-1).astype(jnp.int32)
    hit_table = (flat_ids[:, None] == jnp.arange(experts, dtype=jnp.int32)[None, :]).astype(jnp.int32)
    earlier = jnp.cumsum(hit_table, axis=0) - hit_table
    slot_rank = lax.optimization_barrier(jnp.sum(earlier * hit_table, axis=1))
    return (flat_ids * capacity + slot_rank).astype(jnp.int32)

def mixer(conv_input, out_gate, in_gate, conv_taps, mixer_proj):
    z_rows = (conv_input.astype(jnp.float32) * in_gate.astype(jnp.float32)).astype(jnp.bfloat16)
    length = z_rows.shape[1]
    padded = jnp.pad(z_rows.astype(jnp.float32), ((0, 0), (KERNEL - 1, 0)))
    conv_sum = jnp.zeros(z_rows.shape, jnp.float32)
    for lag_index in range(KERNEL):
        begin = KERNEL - 1 - lag_index
        conv_sum = conv_sum + conv_taps[lag_index][:, None] * padded[:, begin:begin + length]
    gated = (out_gate.astype(jnp.float32) * conv_sum).astype(jnp.bfloat16)
    return jnp.dot(gated.T, mixer_proj, preferred_element_type=jnp.float32).astype(jnp.bfloat16)

def expert_block(inputs):
    rows_in, gate_weight, up_weight, down_weight = inputs
    values = rows_in.astype(jnp.float32)
    row_scale = lax.rsqrt(lax.optimization_barrier(jnp.mean(values * values, axis=1, keepdims=True)) + EPSILON)
    gate_sum = row_scale * jnp.dot(rows_in, gate_weight, preferred_element_type=jnp.float32)
    up_sum = row_scale * jnp.dot(rows_in, up_weight, preferred_element_type=jnp.float32)
    hidden = (jax.nn.silu(gate_sum) * up_sum).astype(jnp.bfloat16)
    split_hidden = hidden.reshape(hidden.shape[0], N_TP, FF_PART).astype(jnp.float32)
    split_down = down_weight.reshape(N_TP, FF_PART, D).astype(jnp.float32)
    partial_value = jnp.einsum('snf,nfd->nsd', split_hidden, split_down).astype(jnp.bfloat16)
    return lax.optimization_barrier(jnp.sum(partial_value.astype(jnp.float32), axis=0)).astype(jnp.bfloat16)

def reference(conv_input, out_gate, in_gate, conv_taps, mixer_proj, token_rows, routes, route_weights, expert_gate, expert_up, expert_down):
    mixed_out = mixer(conv_input, out_gate, in_gate, conv_taps, mixer_proj)
    blocks = TOK_B // ROWS_B
    route_blocks = routes.reshape(blocks, ROWS_B, 2)

    def block_places(route_ids):
        return slot_places(route_ids, CAP, EXPERTS)
    places = jax.vmap(block_places)(route_blocks)
    sources = jnp.arange(2 * ROWS_B, dtype=jnp.int32) // 2

    def fill(rows_in, place_list):
        return jnp.zeros((EXPERTS * CAP, D), jnp.bfloat16).at[place_list].set(rows_in[sources])
    buffers = jax.vmap(fill)(token_rows.reshape(blocks, ROWS_B, D), places)
    by_expert = buffers.reshape(blocks, EXPERTS, CAP, D).transpose(1, 0, 2, 3).reshape(EXPERTS, blocks * CAP, D)
    results = lax.map(expert_block, (by_expert, expert_gate, expert_up, expert_down))
    home = results.reshape(EXPERTS, blocks, CAP, D).transpose(1, 0, 2, 3).reshape(blocks, EXPERTS * CAP, D)

    def pick(rows_in, place_list):
        return rows_in[place_list]
    picked = jax.vmap(pick)(home, places).astype(jnp.float32).reshape(blocks, ROWS_B, 2, D)
    weights = route_weights.reshape(blocks, ROWS_B, 2, 1)
    expert_out = lax.optimization_barrier(jnp.sum(picked * weights, axis=2)).reshape(TOK_B, D).astype(jnp.bfloat16)
    return (mixed_out, expert_out)
```

```python
import jax
import jax.numpy as jnp
from jax import lax
from jax.experimental import pallas as pl
from jax.experimental.pallas import tpu as pltpu
from jax.sharding import PartitionSpec as P

MESH = pl.DeviceIdType.MESH
EPSILON = 1e-06
F32 = jnp.float32
BF16 = jnp.bfloat16

NZ = 16
NCH = 4
OFFS = [0, 1, 15, 2, 14, 3, 13, 4, 12, 5, 11, 6, 10, 7, 9, 8]
ORDER = {o: n for n, o in enumerate(OFFS)}

PLAN = [
    "M1", "P", "M1", "G0", "P", "M0", "G0", "G1", "M1", "G0", "M0", "G2", "G3", "G1", "G0", "G2",
    "G3", "G1", "G3", "G1", "G2", "G0", "G1", "G3", "S1", "S0", "G2", "G3", "S3", "S1", "G2", "S2",
    "S3", "S1", "S2", "S1", "S3", "S0", "P", "S2", "S3", "S1", "M0", "S0", "S2", "M1", "S3", "M0",
    "S0", "P", "S2", "M1", "M0", "S0", "M1", "M0", "M0", "M1",
]
M_GROUP = [0, 1, 1, 2, 3, 4, 5, 5]


def body(conv_in, out_gate, in_gate, taps, proj, tokens, routes, weights, wg, wu, wd,
         mixed_ref, out_ref,
         ci_v, og_v, ig_v, wg_v, wu_v, wd_v, z_v, halo_v, taps_v, px, py,
         ysrc, yq, yt, oq, ot, mix, disp, xg, part, er, ret, r1, r2, r3, r4,
         load_sem, d_send, d_recv, r_send, r_recv, ag_send, ag_recv, rs_send, rs_recv, m_send, m_recv,
         p_send, p_recv, h_sem, own_sem):
    ep = lax.axis_index("ep")
    tp = lax.axis_index("tp")
    z, c = ep // 2, ep % 2
    y, x = tp // 4, tp % 4
    xm, xp, ym, yp = (x + 3) % 4, (x + 1) % 4, (y + 3) % 4, (y + 1) % 4
    x2, y2 = (x + 2) % 4, (y + 2) % 4
    near = {"x+": (ep, y * 4 + xp), "x-": (ep, y * 4 + xm), "y+": (ep, yp * 4 + x), "y-": (ep, ym * 4 + x)}

    def ep_at(dz, dc):
        return ((z + dz) % NZ) * 2 + (c + dc) % 2

    barrier = pltpu.get_barrier_semaphore()
    for dev in near.values():
        pl.semaphore_signal(barrier, inc=1, device_id=dev, device_id_type=MESH)
    for dz in range(NZ):
        for dc in range(2):
            if dz or dc:
                pl.semaphore_signal(barrier, inc=1, device_id=(ep_at(dz, dc), tp), device_id_type=MESH)

    half = pl.ds(pl.multiple_of(c * 512, 512), 512)
    loads = {}
    for n, (name, src, dst) in enumerate([
        ("px", proj.at[half], px.at[x, half]), ("py", proj.at[half], py.at[y, half]),
        ("ci", conv_in, ci_v), ("ig", in_gate, ig_v), ("og", out_gate, og_v),
        ("wg", wg.at[0], wg_v), ("wu", wu.at[0], wu_v), ("wd", wd.at[0], wd_v),
    ]):
        loads[name] = pltpu.make_async_copy(src, dst, load_sem.at[n])
        loads[name].start()

    r_all = routes[...].astype(F32)
    r0, r1_ = r_all[0:1, :], r_all[1:2, :]
    eidx = lax.broadcasted_iota(jnp.int32, (32, 256), 0).astype(F32)
    eq0, eq1 = eidx == r0, eidx == r1_
    hit = jnp.where(eq0, 1.0, 0.0) + jnp.where(eq1, 1.0, 0.0)
    before = lax.broadcasted_iota(jnp.int32, (256, 256), 0) < lax.broadcasted_iota(jnp.int32, (256, 256), 1)
    earlier = jnp.dot(hit.astype(BF16), jnp.where(before, 1.0, 0.0).astype(BF16), preferred_element_type=F32)
    p0 = r0 * 32.0 + jnp.sum(jnp.where(eq0, earlier, 0.0), axis=0, keepdims=True)
    p1 = r1_ * 32.0 + jnp.sum(jnp.where(eq1, earlier, 0.0), axis=0, keepdims=True)
    slot = lax.broadcasted_iota(jnp.int32, (1024, 256), 0).astype(F32)
    onehot = jnp.where((slot == p0) | (slot == p1), 1.0, 0.0).astype(BF16)
    disp[...] = jnp.dot(onehot, tokens[...], preferred_element_type=F32).astype(BF16).reshape(32, 32, 128)

    loads["ci"].wait()
    loads["ig"].wait()
    z_v[...] = (ci_v[...].astype(F32) * ig_v[...].astype(F32)).astype(BF16)
    pl.semaphore_wait(barrier, 35)
    halo = pltpu.make_async_remote_copy(
        z_v.at[:, 1920:2048], halo_v, h_sem.at[0], h_sem.at[1],
        device_id=((ep + 1) % 32, tp), device_id_type=MESH)
    halo.start()

    own_in = pltpu.make_async_copy(disp.at[ep], xg.at[0, y, x, 0], own_sem.at[0])
    own_in.start()
    for off in OFFS:
        for dc in range(2):
            if off == 0 and dc == 0:
                continue
            pos = ORDER[off] * 2 + dc
            dst = ep_at((NZ - off) % NZ, dc)
            pltpu.make_async_remote_copy(
                disp.at[dst], xg.at[pos // 8, y, x, pos % 8], d_send.at[0], d_recv.at[pos // 8],
                device_id=(dst, tp), device_id_type=MESH).start()

    tap_rows = jnp.concatenate([taps[...], jnp.zeros((125, 1024), F32)], axis=0)
    taps_v[...] = tap_rows.T
    t_all = taps_v[pl.ds(pl.multiple_of(tp * 64, 64), 64), :]
    t0, t1, t2 = t_all[:, 0:1], t_all[:, 1:2], t_all[:, 2:3]
    loads["og"].wait()

    def make_y(n):
        here = z_v[:, n * 512:(n + 1) * 512].astype(F32)
        if n:
            edge = z_v[:, n * 512 - 128:n * 512].astype(F32)
        else:
            edge = jnp.where(ep > 0, halo_v[...].astype(F32), 0.0)
        longer = jnp.concatenate([edge, here], axis=1)
        conv = t0 * here + t1 * pltpu.roll(longer, 1, 1)[:, 128:] + t2 * pltpu.roll(longer, 2, 1)[:, 128:]
        gated = (og_v[:, n * 512:(n + 1) * 512].astype(F32) * conv).astype(BF16)
        for g in range(4):
            ysrc[n, g] = gated[:, g * 128:(g + 1) * 128]
        yq[n, y, x] = ysrc[n, y if n % 2 else x]

    def start(copies):
        for cp in copies:
            cp.start()

    def arrived(ref, sem):
        pltpu.make_async_remote_copy(ref, ref, h_sem.at[0], sem, device_id=near["x+"], device_id_type=MESH).wait_recv()

    def left(ref, sem):
        pltpu.make_async_remote_copy(ref, ref, sem, h_sem.at[1], device_id=near["x+"], device_id_type=MESH).wait_send()

    def gather(buf, size, job):
        h, q = size // 2, size // 4
        def send(n, ref, way):
            return pltpu.make_async_remote_copy(
                ref, ref, ag_send.at[n // 8], ag_recv.at[job, n // 4], device_id=near[way], device_id_type=MESH)
        start([
            send(0, buf.at[y, x, 0:h], "x+"), send(1, buf.at[y, x, 0:h], "x-"),
            send(2, buf.at[y, x, h:size], "y+"), send(3, buf.at[y, x, h:size], "y-")])
        yield
        arrived(buf.at[0, 0:2], ag_recv.at[job, 0])
        start([
            send(4, buf.at[y, xm, 0:q], "x+"), send(5, buf.at[y, xp, q:h], "x-"),
            send(6, buf.at[ym, x, h:h + q], "y+"), send(7, buf.at[yp, x, h + q:size], "y-")])
        yield
        arrived(buf.at[0, 0], ag_recv.at[job, 1])
        start([
            send(8, buf.at[y, :, 0:h], "y+"), send(9, buf.at[y, :, 0:h], "y-"),
            send(10, buf.at[:, x, h:size], "x+"), send(11, buf.at[:, x, h:size], "x-")])
        yield
        arrived(buf.at[0:2], ag_recv.at[job, 2])
        start([
            send(12, buf.at[ym, :, 0:q], "y+"), send(13, buf.at[yp, :, q:h], "y-"),
            send(14, buf.at[:, xm, h:h + q], "x+"), send(15, buf.at[:, xp, h + q:size], "x-")])
        yield
        arrived(buf.at[0], ag_recv.at[job, 3])

    def proj_job():
        lo = pl.ds(pl.multiple_of(c * 512, 512), 256)
        hi = pl.ds(pl.multiple_of(c * 512 + 256, 256), 256)
        partner = (z * 2 + (c + 1) % 2, tp)

        def send(n, ref, dev):
            return pltpu.make_async_remote_copy(
                ref, ref, p_send.at[n // 8], p_recv.at[n // 4], device_id=dev, device_id_type=MESH)

        loads["px"].wait()
        loads["py"].wait()
        start([
            send(0, px.at[x, half], near["x+"]), send(1, px.at[x, half], near["x-"]),
            send(2, py.at[y, half], near["y+"]), send(3, py.at[y, half], near["y-"])])
        yield
        arrived(px.at[0:2], p_recv.at[0])
        start([
            send(4, px.at[xm, lo], near["x+"]), send(5, px.at[xp, hi], near["x-"]),
            send(6, py.at[ym, lo], near["y+"]), send(7, py.at[yp, hi], near["y-"])])
        yield
        arrived(px.at[0], p_recv.at[1])
        start([send(8, px.at[:, half], partner), send(9, py.at[:, half], partner)])
        yield
        arrived(px, p_recv.at[2])
        yield

    def mixer_job(n):
        a, b = 2 * n, 2 * n + 1
        if n == 0:
            halo.wait_recv()
        make_y(a)
        make_y(b)

        def send(m, src, dst, way):
            return pltpu.make_async_remote_copy(
                src, dst, m_send.at[n], m_recv.at[n, M_GROUP[m // 4]], device_id=near[way], device_id_type=MESH)

        start([
            send(0, ysrc.at[a, x2, 0:32], yt.at[a, 0], "x+"), send(1, ysrc.at[a, x2, 32:64], yt.at[a, 1], "x-"),
            send(2, ysrc.at[b, y2, 0:32], yt.at[b, 0], "y+"), send(3, ysrc.at[b, y2, 32:64], yt.at[b, 1], "y-")])
        start([
            send(4, ysrc.at[a, xp], yq.at[a, y, x], "x+"), send(5, ysrc.at[a, xm], yq.at[a, y, x], "x-"),
            send(6, ysrc.at[b, yp], yq.at[b, y, x], "y+"), send(7, ysrc.at[b, ym], yq.at[b, y, x], "y-")])
        yield
        arrived(yq.at[a, 0, 0:2], m_recv.at[n, 0])
        start([
            send(8, yt.at[a, 0], yq.at[a, y, xm, 0:32], "x+"), send(9, yt.at[a, 1], yq.at[a, y, xp, 32:64], "x-"),
            send(10, yt.at[b, 0], yq.at[b, ym, x, 0:32], "y+"), send(11, yt.at[b, 1], yq.at[b, yp, x, 32:64], "y-")])
        yield
        arrived(yq.at[a, 0:2, 0:3], m_recv.at[n, 1])
        start([
            send(12, yq.at[a, y], yq.at[a, y], "y+"), send(13, yq.at[a, y], yq.at[a, y], "y-"),
            send(14, yq.at[b, :, x], yq.at[b, :, x], "x+"), send(15, yq.at[b, :, x], yq.at[b, :, x], "x-")])
        yield
        arrived(yq.at[a], m_recv.at[n, 2])
        start([
            send(16, yq.at[a, ym, :, 0:32], yq.at[a, ym, :, 0:32], "y+"),
            send(17, yq.at[a, yp, :, 32:64], yq.at[a, yp, :, 32:64], "y-"),
            send(18, yq.at[b, :, xm, 0:32], yq.at[b, :, xm, 0:32], "x+"),
            send(19, yq.at[b, :, xp, 32:64], yq.at[b, :, xp, 32:64], "x-")])
        yield
        arrived(yq.at[a, 0:2], m_recv.at[n, 3])
        for k, pw in ((a, px), (b, py)):
            full = jnp.concatenate([yq[k, i, j] for i in range(4) for j in range(4)], axis=0)
            rows = full.astype(F32).T.astype(BF16)
            block = jnp.dot(rows, jnp.concatenate([pw[g] for g in range(4)], axis=1),
                            preferred_element_type=F32).astype(BF16)
            for g in range(4):
                oq[k, g] = block[:, g * 128:(g + 1) * 128]
            mine = y if k % 2 else x
            mix[k, mine] = oq[k, mine]
        start([
            send(20, oq.at[a, x2, 0:64], ot.at[a, 0], "x+"), send(21, oq.at[a, x2, 64:128], ot.at[a, 1], "x-"),
            send(22, oq.at[b, y2, 0:64], ot.at[b, 0], "y+"), send(23, oq.at[b, y2, 64:128], ot.at[b, 1], "y-")])
        start([
            send(24, oq.at[a, xp], mix.at[a, x], "x+"), send(25, oq.at[a, xm], mix.at[a, x], "x-"),
            send(26, oq.at[b, yp], mix.at[b, y], "y+"), send(27, oq.at[b, ym], mix.at[b, y], "y-")])
        yield
        arrived(yq.at[a, 0], m_recv.at[n, 4])
        start([
            send(28, ot.at[a, 0], mix.at[a, xm, 0:64], "x+"), send(29, ot.at[a, 1], mix.at[a, xp, 64:128], "x-"),
            send(30, ot.at[b, 0], mix.at[b, ym, 0:64], "y+"), send(31, ot.at[b, 1], mix.at[b, yp, 64:128], "y-")])
        yield
        arrived(yq.at[a, 0:3], m_recv.at[n, 5])
        for k in (a, b):
            mixed_ref[k * 512:(k + 1) * 512, :] = mix[k].reshape(512, 128)
        yield

    def gather_job(n):
        if n == 0:
            own_in.wait()
        arrived(xg.at[n, 0, 0, 0:7 if n == 0 else 8], d_recv.at[n])
        yield from gather(xg.at[n], 8, n)
        yield

    def experts(n):
        if "wg" in loads:
            for name in ("wg", "wu", "wd"):
                loads.pop(name).wait()
        cols = [xg[n, i, j].reshape(256, 128) for i in range(4) for j in range(4)]
        squares = jnp.square(cols[0].astype(F32))
        for col in cols[1:]:
            squares = squares + jnp.square(col.astype(F32))
        scale = lax.rsqrt(jnp.sum(squares, axis=1, keepdims=True) / 2048.0 + EPSILON)
        rows = jnp.concatenate(cols, axis=1)
        gate = scale * jnp.dot(rows, wg_v[...], preferred_element_type=F32)
        up = scale * jnp.dot(rows, wu_v[...], preferred_element_type=F32)
        hidden = (gate * (1.0 / (1.0 + jnp.exp(-gate))) * up).astype(BF16)
        for i in range(4):
            block = jnp.dot(hidden, wd_v[:, i * 512:(i + 1) * 512], preferred_element_type=F32).astype(BF16)
            for j in range(4):
                part[n, i, j] = block[:, j * 128:(j + 1) * 128].reshape(8, 32, 128)

    def add(*refs):
        total = refs[0][...].astype(F32)
        for ref in refs[1:]:
            total = total + ref[...].astype(F32)
        return total.astype(BF16)

    own_out = pltpu.make_async_copy(er.at[0, 0], ret.at[ep], own_sem.at[1])

    def scatter_job(n):
        experts(n)
        buf = part.at[n]

        def send(m, src, dst, way):
            return pltpu.make_async_remote_copy(
                src, dst, rs_send.at[m // 8], rs_recv.at[n, m // 4], device_id=near[way], device_id_type=MESH)

        start([
            send(0, buf.at[y2, :, 0:2], r1.at[n, 0], "y+"), send(1, buf.at[y2, :, 2:4], r1.at[n, 1], "y-"),
            send(2, buf.at[:, x2, 4:6], r1.at[n, 2], "x+"), send(3, buf.at[:, x2, 6:8], r1.at[n, 3], "x-")])
        yield
        arrived(buf.at[0], rs_recv.at[n, 0])
        buf[yp, :, 0:2] = add(buf.at[yp, :, 0:2], r1.at[n, 0])
        buf[ym, :, 2:4] = add(buf.at[ym, :, 2:4], r1.at[n, 1])
        buf[:, xp, 4:6] = add(buf.at[:, xp, 4:6], r1.at[n, 2])
        buf[:, xm, 6:8] = add(buf.at[:, xm, 6:8], r1.at[n, 3])
        start([
            send(4, buf.at[yp, :, 0:4], r2.at[n, 0], "y+"), send(5, buf.at[ym, :, 0:4], r2.at[n, 1], "y-"),
            send(6, buf.at[:, xp, 4:8], r2.at[n, 2], "x+"), send(7, buf.at[:, xm, 4:8], r2.at[n, 3], "x-")])
        yield
        arrived(buf.at[0:2], rs_recv.at[n, 1])
        buf[y, :, 0:4] = add(buf.at[y, :, 0:4], r2.at[n, 0], r2.at[n, 1])
        buf[:, x, 4:8] = add(buf.at[:, x, 4:8], r2.at[n, 2], r2.at[n, 3])
        start([
            send(8, buf.at[y, x2, 0:2], r3.at[n, 0], "x+"), send(9, buf.at[y, x2, 2:4], r3.at[n, 1], "x-"),
            send(10, buf.at[y2, x, 4:6], r3.at[n, 2], "y+"), send(11, buf.at[y2, x, 6:8], r3.at[n, 3], "y-")])
        yield
        arrived(buf.at[0, 0], rs_recv.at[n, 2])
        buf[y, xp, 0:2] = add(buf.at[y, xp, 0:2], r3.at[n, 0])
        buf[y, xm, 2:4] = add(buf.at[y, xm, 2:4], r3.at[n, 1])
        buf[yp, x, 4:6] = add(buf.at[yp, x, 4:6], r3.at[n, 2])
        buf[ym, x, 6:8] = add(buf.at[ym, x, 6:8], r3.at[n, 3])
        start([
            send(12, buf.at[y, xp, 0:4], r4.at[n, 0], "x+"), send(13, buf.at[y, xm, 0:4], r4.at[n, 1], "x-"),
            send(14, buf.at[yp, x, 4:8], r4.at[n, 2], "y+"), send(15, buf.at[ym, x, 4:8], r4.at[n, 3], "y-")])
        yield
        arrived(buf.at[0, 0:2], rs_recv.at[n, 3])
        er[n, 0:4] = add(buf.at[y, x, 0:4], r4.at[n, 0], r4.at[n, 1])
        er[n, 4:8] = add(buf.at[y, x, 4:8], r4.at[n, 2], r4.at[n, 3])
        for pos in reversed(range(n * 8, n * 8 + 8)):
            if pos == 0:
                own_out.start()
                continue
            dst = ep_at(OFFS[pos // 2], pos % 2)
            pltpu.make_async_remote_copy(
                er.at[n, pos % 8], ret.at[ep], r_send.at[0], r_recv.at[0],
                device_id=(dst, tp), device_id_type=MESH).start()
        yield

    jobs = {"P": proj_job(), "M0": mixer_job(0), "M1": mixer_job(1)}
    for n in range(NCH):
        jobs[f"G{n}"] = gather_job(n)
        jobs[f"S{n}"] = scatter_job(n)
    for item in PLAN:
        next(jobs[item])

    row = lax.broadcasted_iota(jnp.int32, (128, 256), 0)
    w_all = weights[...]
    table = jnp.where(row == 0, p0, 0.0) + jnp.where(row == 1, p1, 0.0)
    table = jnp.where(row == 2, w_all[0:1, :], table)
    table = jnp.where(row == 3, w_all[1:2, :], table)
    cols = table.T
    slot_t = lax.broadcasted_iota(jnp.int32, (256, 1024), 1).astype(F32)
    pick0 = jnp.where(slot_t == cols[:, 0:1], 1.0, 0.0).astype(BF16)
    pick1 = jnp.where(slot_t == cols[:, 1:2], 1.0, 0.0).astype(BF16)
    own_out.wait()
    arrived(ret.at[0:31], r_recv.at[0])
    home = ret[...].reshape(1024, 128)
    out_ref[...] = (cols[:, 2:3] * jnp.dot(pick0, home, preferred_element_type=F32)
                    + cols[:, 3:4] * jnp.dot(pick1, home, preferred_element_type=F32)).astype(BF16)
    halo.wait_send()
    left(disp.at[0:31], d_send.at[0])
    left(ret.at[0:31], r_send.at[0])
    left(xg.at[0, 0:3], ag_send.at[0])
    left(xg.at[0:3], ag_send.at[1])
    left(part.at[0:3], rs_send.at[0])
    left(part.at[0, 0:3], rs_send.at[1])
    left(px.at[0:3], p_send.at[0])
    left(px, p_send.at[1])
    left(px.at[0:3], m_send.at[0])
    left(px.at[0:3], m_send.at[1])


def step(conv_input, out_gate, in_gate, conv_taps, mixer_proj, token_rows, routes, route_weights,
         expert_gate, expert_up, expert_down):
    vmem = pl.BlockSpec(memory_space=pltpu.VMEM)
    hbm = pl.BlockSpec(memory_space=pl.ANY)
    dma = pltpu.SemaphoreType.DMA
    return pl.pallas_call(
        body,
        out_shape=(jax.ShapeDtypeStruct((2048, 128), BF16), jax.ShapeDtypeStruct((256, 128), BF16)),
        in_specs=[hbm, hbm, hbm, vmem, hbm, vmem, vmem, vmem, hbm, hbm, hbm],
        out_specs=(vmem, vmem),
        scratch_shapes=[
            pltpu.VMEM((64, 2048), BF16), pltpu.VMEM((64, 2048), BF16), pltpu.VMEM((64, 2048), BF16),
            pltpu.VMEM((2048, 256), BF16), pltpu.VMEM((2048, 256), BF16), pltpu.VMEM((256, 2048), BF16),
            pltpu.VMEM((64, 2048), BF16), pltpu.VMEM((64, 128), BF16), pltpu.VMEM((1024, 128), F32),
            pltpu.VMEM((4, 1024, 128), BF16), pltpu.VMEM((4, 1024, 128), BF16),
            pltpu.VMEM((4, 4, 64, 128), BF16), pltpu.VMEM((4, 4, 4, 64, 128), BF16),
            pltpu.VMEM((4, 2, 32, 128), BF16), pltpu.VMEM((4, 4, 128, 128), BF16),
            pltpu.VMEM((4, 2, 64, 128), BF16), pltpu.VMEM((4, 4, 128, 128), BF16),
            pltpu.VMEM((32, 32, 128), BF16),
            pltpu.VMEM((NCH, 4, 4, 8, 32, 128), BF16),
            pltpu.VMEM((NCH, 4, 4, 8, 32, 128), BF16),
            pltpu.VMEM((NCH, 8, 32, 128), BF16),
            pltpu.VMEM((32, 32, 128), BF16),
            pltpu.VMEM((NCH, 4, 4, 2, 32, 128), BF16),
            pltpu.VMEM((NCH, 4, 4, 4, 32, 128), BF16),
            pltpu.VMEM((NCH, 4, 2, 32, 128), BF16),
            pltpu.VMEM((NCH, 4, 4, 32, 128), BF16),
            dma((8,)), dma((1,)), dma((NCH,)), dma((1,)), dma((1,)),
            dma((2,)), dma((NCH, 4)), dma((2,)), dma((NCH, 4)), dma((2,)), dma((2, 6)),
            dma((2,)), dma((3,)), dma((2,)), dma((2,)),
        ],
        compiler_params=pltpu.CompilerParams(
            collective_id=0, has_side_effects=True, vmem_limit_bytes=60 * 1024 * 1024),
    )(conv_input, out_gate, in_gate, conv_taps, mixer_proj, token_rows, routes.T, route_weights.T,
      expert_gate, expert_up, expert_down)


def solution(mesh):
    return jax.shard_map(
        step,
        mesh=mesh,
        in_specs=(
            P("tp", "ep"), P("tp", "ep"), P("tp", "ep"), P(), P(None, "tp"), P("ep", "tp"),
            P("ep", None), P("ep", None), P("ep", None, "tp"), P("ep", None, "tp"), P("ep", "tp", None),
        ),
        out_specs=(P("ep", "tp"), P("ep", "tp")),
        check_vma=False,
    )
```

```python
import jax
import jax.numpy as jnp
from jax import lax
from jax.experimental import pallas as pl
from jax.experimental.pallas import tpu as pltpu
from jax.sharding import PartitionSpec as P

MESH = pl.DeviceIdType.MESH
EPSILON = 1e-06
F32 = jnp.float32
BF16 = jnp.bfloat16

NZ = 16
NCH = 4
OFFS = [0, 1, 15, 2, 14, 3, 13, 4, 12, 5, 11, 6, 10, 7, 9, 8]
ORDER = {o: n for n, o in enumerate(OFFS)}

PLAN = [
    "D", "P", "M1", "M0", "M0", "M1", "P", "G0", "M0", "G0", "G1", "M1", "G0", "G1", "G2", "G3",
    "M1", "G0", "G2", "G3", "G1", "G3", "G1", "G2", "G1", "G3", "S1", "G0", "G2", "S0", "G3", "P",
    "S3", "G2", "S1", "S2", "S3", "S1", "S2", "S1", "S3", "S0", "S1", "S2", "S3", "M0", "S0", "P",
    "S2", "M1", "S3", "S0", "S2", "M0", "S0", "M1", "M0", "M0", "M1",
]
M_GROUP = [0, 1, 1, 2, 3, 4, 5, 5]


def body(conv_in, out_gate, in_gate, taps, proj, tokens, routes, weights, wg, wu, wd,
         mixed_ref, out_ref,
         ci_v, og_v, ig_v, wg_v, wu_v, wd_v, z_v, halo_v, taps_v, px, py,
         ysrc, yq, yt, oq, ot, mix, disp, xg, part, er, ret, r1, r2, r3, r4,
         load_sem, d_send, d_recv, r_send, r_recv, ag_send, ag_recv, rs_send, rs_recv, m_send, m_recv,
         p_send, p_recv, h_sem, own_sem):
    ep = lax.axis_index("ep")
    tp = lax.axis_index("tp")
    z, c = ep // 2, ep % 2
    y, x = tp // 4, tp % 4
    xm, xp, ym, yp = (x + 3) % 4, (x + 1) % 4, (y + 3) % 4, (y + 1) % 4
    x2, y2 = (x + 2) % 4, (y + 2) % 4
    near = {"x+": (ep, y * 4 + xp), "x-": (ep, y * 4 + xm), "y+": (ep, yp * 4 + x), "y-": (ep, ym * 4 + x)}

    def ep_at(dz, dc):
        return ((z + dz) % NZ) * 2 + (c + dc) % 2

    barrier = pltpu.get_barrier_semaphore()
    for dev in near.values():
        pl.semaphore_signal(barrier, inc=1, device_id=dev, device_id_type=MESH)
    for dz in range(NZ):
        for dc in range(2):
            if dz or dc:
                pl.semaphore_signal(barrier, inc=1, device_id=(ep_at(dz, dc), tp), device_id_type=MESH)

    half = pl.ds(pl.multiple_of(c * 512, 512), 512)
    loads = {}
    for n, (name, src, dst) in enumerate([
        ("px", proj.at[half], px.at[x, half]), ("py", proj.at[half], py.at[y, half]),
        ("ci", conv_in, ci_v), ("ig", in_gate, ig_v), ("og", out_gate, og_v),
        ("wg", wg.at[0], wg_v), ("wu", wu.at[0], wu_v), ("wd", wd.at[0], wd_v),
    ]):
        loads[name] = pltpu.make_async_copy(src, dst, load_sem.at[n])
        loads[name].start()

    r_all = routes[...].astype(F32)
    r0, r1_ = r_all[0:1, :], r_all[1:2, :]
    eidx = lax.broadcasted_iota(jnp.int32, (32, 256), 0).astype(F32)
    eq0, eq1 = eidx == r0, eidx == r1_
    hit = jnp.where(eq0, 1.0, 0.0) + jnp.where(eq1, 1.0, 0.0)
    before = lax.broadcasted_iota(jnp.int32, (256, 256), 0) < lax.broadcasted_iota(jnp.int32, (256, 256), 1)
    earlier = jnp.dot(hit.astype(BF16), jnp.where(before, 1.0, 0.0).astype(BF16), preferred_element_type=F32)
    p0 = r0 * 32.0 + jnp.sum(jnp.where(eq0, earlier, 0.0), axis=0, keepdims=True)
    p1 = r1_ * 32.0 + jnp.sum(jnp.where(eq1, earlier, 0.0), axis=0, keepdims=True)
    slot = lax.broadcasted_iota(jnp.int32, (1024, 256), 0).astype(F32)
    onehot = jnp.where((slot == p0) | (slot == p1), 1.0, 0.0).astype(BF16)
    disp[...] = jnp.dot(onehot, tokens[...], preferred_element_type=F32).astype(BF16).reshape(32, 32, 128)

    tap_rows = jnp.concatenate([taps[...], jnp.zeros((125, 1024), F32)], axis=0)
    taps_v[...] = tap_rows.T
    t_all = taps_v[pl.ds(pl.multiple_of(tp * 64, 64), 64), :]
    t0, t1, t2 = t_all[:, 0:1], t_all[:, 1:2], t_all[:, 2:3]
    loads["ci"].wait()
    loads["ig"].wait()
    z_v[...] = (ci_v[...].astype(F32) * ig_v[...].astype(F32)).astype(BF16)
    loads["og"].wait()

    def make_y(n):
        here = z_v[:, n * 512:(n + 1) * 512].astype(F32)
        if n:
            edge = z_v[:, n * 512 - 128:n * 512].astype(F32)
        else:
            edge = jnp.where(ep > 0, halo_v[...].astype(F32), 0.0)
        longer = jnp.concatenate([edge, here], axis=1)
        conv = t0 * here + t1 * pltpu.roll(longer, 1, 1)[:, 128:] + t2 * pltpu.roll(longer, 2, 1)[:, 128:]
        gated = (og_v[:, n * 512:(n + 1) * 512].astype(F32) * conv).astype(BF16)
        for g in range(4):
            ysrc[n, g] = gated[:, g * 128:(g + 1) * 128]
        yq[n, y, x] = ysrc[n, y if n % 2 else x]

    for n in range(1, NCH):
        make_y(n)

    pl.semaphore_wait(barrier, 35)

    halo = pltpu.make_async_remote_copy(
        z_v.at[:, 1920:2048], halo_v, h_sem.at[0], h_sem.at[1],
        device_id=((ep + 1) % 32, tp), device_id_type=MESH)
    own_in = pltpu.make_async_copy(disp.at[ep], xg.at[0, y, x, 0], own_sem.at[0])

    def dispatch_job():
        halo.start()
        own_in.start()
        for off in OFFS:
            for dc in range(2):
                if off == 0 and dc == 0:
                    continue
                pos = ORDER[off] * 2 + dc
                dst = ep_at((NZ - off) % NZ, dc)
                pltpu.make_async_remote_copy(
                    disp.at[dst], xg.at[pos // 8, y, x, pos % 8], d_send.at[0], d_recv.at[pos // 8],
                    device_id=(dst, tp), device_id_type=MESH).start()
        yield

    def start(copies):
        for cp in copies:
            cp.start()

    def arrived(ref, sem):
        pltpu.make_async_remote_copy(ref, ref, h_sem.at[0], sem, device_id=near["x+"], device_id_type=MESH).wait_recv()

    def left(ref, sem):
        pltpu.make_async_remote_copy(ref, ref, sem, h_sem.at[1], device_id=near["x+"], device_id_type=MESH).wait_send()

    def gather(buf, size, job):
        h, q = size // 2, size // 4
        def send(n, ref, way):
            return pltpu.make_async_remote_copy(
                ref, ref, ag_send.at[n // 8], ag_recv.at[job, n // 4], device_id=near[way], device_id_type=MESH)
        start([
            send(0, buf.at[y, x, 0:h], "x+"), send(1, buf.at[y, x, 0:h], "x-"),
            send(2, buf.at[y, x, h:size], "y+"), send(3, buf.at[y, x, h:size], "y-")])
        yield
        arrived(buf.at[0, 0:2], ag_recv.at[job, 0])
        start([
            send(4, buf.at[y, xm, 0:q], "x+"), send(5, buf.at[y, xp, q:h], "x-"),
            send(6, buf.at[ym, x, h:h + q], "y+"), send(7, buf.at[yp, x, h + q:size], "y-")])
        yield
        arrived(buf.at[0, 0], ag_recv.at[job, 1])
        start([
            send(8, buf.at[y, :, 0:h], "y+"), send(9, buf.at[y, :, 0:h], "y-"),
            send(10, buf.at[:, x, h:size], "x+"), send(11, buf.at[:, x, h:size], "x-")])
        yield
        arrived(buf.at[0:2], ag_recv.at[job, 2])
        start([
            send(12, buf.at[ym, :, 0:q], "y+"), send(13, buf.at[yp, :, q:h], "y-"),
            send(14, buf.at[:, xm, h:h + q], "x+"), send(15, buf.at[:, xp, h + q:size], "x-")])
        yield
        arrived(buf.at[0], ag_recv.at[job, 3])

    def proj_job():
        lo = pl.ds(pl.multiple_of(c * 512, 512), 256)
        hi = pl.ds(pl.multiple_of(c * 512 + 256, 256), 256)
        partner = (z * 2 + (c + 1) % 2, tp)

        def send(n, ref, dev):
            return pltpu.make_async_remote_copy(
                ref, ref, p_send.at[n // 8], p_recv.at[n // 4], device_id=dev, device_id_type=MESH)

        loads["px"].wait()
        loads["py"].wait()
        start([
            send(0, px.at[x, half], near["x+"]), send(1, px.at[x, half], near["x-"]),
            send(2, py.at[y, half], near["y+"]), send(3, py.at[y, half], near["y-"])])
        yield
        arrived(px.at[0:2], p_recv.at[0])
        start([
            send(4, px.at[xm, lo], near["x+"]), send(5, px.at[xp, hi], near["x-"]),
            send(6, py.at[ym, lo], near["y+"]), send(7, py.at[yp, hi], near["y-"])])
        yield
        arrived(px.at[0], p_recv.at[1])
        start([send(8, px.at[:, half], partner), send(9, py.at[:, half], partner)])
        yield
        arrived(px, p_recv.at[2])
        yield

    def mixer_job(n):
        a, b = 2 * n, 2 * n + 1
        if n == 0:
            halo.wait_recv()
            make_y(0)

        def send(m, src, dst, way):
            return pltpu.make_async_remote_copy(
                src, dst, m_send.at[n], m_recv.at[n, M_GROUP[m // 4]], device_id=near[way], device_id_type=MESH)

        start([
            send(0, ysrc.at[a, x2, 0:32], yt.at[a, 0], "x+"), send(1, ysrc.at[a, x2, 32:64], yt.at[a, 1], "x-"),
            send(2, ysrc.at[b, y2, 0:32], yt.at[b, 0], "y+"), send(3, ysrc.at[b, y2, 32:64], yt.at[b, 1], "y-")])
        start([
            send(4, ysrc.at[a, xp], yq.at[a, y, x], "x+"), send(5, ysrc.at[a, xm], yq.at[a, y, x], "x-"),
            send(6, ysrc.at[b, yp], yq.at[b, y, x], "y+"), send(7, ysrc.at[b, ym], yq.at[b, y, x], "y-")])
        yield
        arrived(yq.at[a, 0, 0:2], m_recv.at[n, 0])
        start([
            send(8, yt.at[a, 0], yq.at[a, y, xm, 0:32], "x+"), send(9, yt.at[a, 1], yq.at[a, y, xp, 32:64], "x-"),
            send(10, yt.at[b, 0], yq.at[b, ym, x, 0:32], "y+"), send(11, yt.at[b, 1], yq.at[b, yp, x, 32:64], "y-")])
        yield
        arrived(yq.at[a, 0:2, 0:3], m_recv.at[n, 1])
        start([
            send(12, yq.at[a, y], yq.at[a, y], "y+"), send(13, yq.at[a, y], yq.at[a, y], "y-"),
            send(14, yq.at[b, :, x], yq.at[b, :, x], "x+"), send(15, yq.at[b, :, x], yq.at[b, :, x], "x-")])
        yield
        arrived(yq.at[a], m_recv.at[n, 2])
        start([
            send(16, yq.at[a, ym, :, 0:32], yq.at[a, ym, :, 0:32], "y+"),
            send(17, yq.at[a, yp, :, 32:64], yq.at[a, yp, :, 32:64], "y-"),
            send(18, yq.at[b, :, xm, 0:32], yq.at[b, :, xm, 0:32], "x+"),
            send(19, yq.at[b, :, xp, 32:64], yq.at[b, :, xp, 32:64], "x-")])
        yield
        arrived(yq.at[a, 0:2], m_recv.at[n, 3])
        for k, pw in ((a, px), (b, py)):
            full = jnp.concatenate([yq[k, i, j] for i in range(4) for j in range(4)], axis=0)
            rows = full.astype(F32).T.astype(BF16)
            block = jnp.dot(rows, jnp.concatenate([pw[g] for g in range(4)], axis=1),
                            preferred_element_type=F32).astype(BF16)
            for g in range(4):
                oq[k, g] = block[:, g * 128:(g + 1) * 128]
            mine = y if k % 2 else x
            mix[k, mine] = oq[k, mine]
        start([
            send(20, oq.at[a, x2, 0:64], ot.at[a, 0], "x+"), send(21, oq.at[a, x2, 64:128], ot.at[a, 1], "x-"),
            send(22, oq.at[b, y2, 0:64], ot.at[b, 0], "y+"), send(23, oq.at[b, y2, 64:128], ot.at[b, 1], "y-")])
        start([
            send(24, oq.at[a, xp], mix.at[a, x], "x+"), send(25, oq.at[a, xm], mix.at[a, x], "x-"),
            send(26, oq.at[b, yp], mix.at[b, y], "y+"), send(27, oq.at[b, ym], mix.at[b, y], "y-")])
        yield
        arrived(yq.at[a, 0], m_recv.at[n, 4])
        start([
            send(28, ot.at[a, 0], mix.at[a, xm, 0:64], "x+"), send(29, ot.at[a, 1], mix.at[a, xp, 64:128], "x-"),
            send(30, ot.at[b, 0], mix.at[b, ym, 0:64], "y+"), send(31, ot.at[b, 1], mix.at[b, yp, 64:128], "y-")])
        yield
        arrived(yq.at[a, 0:3], m_recv.at[n, 5])
        for k in (a, b):
            mixed_ref[k * 512:(k + 1) * 512, :] = mix[k].reshape(512, 128)
        yield

    def gather_job(n):
        if n == 0:
            own_in.wait()
        arrived(xg.at[n, 0, 0, 0:7 if n == 0 else 8], d_recv.at[n])
        yield from gather(xg.at[n], 8, n)
        yield

    def experts(n):
        if "wg" in loads:
            for name in ("wg", "wu", "wd"):
                loads.pop(name).wait()
        cols = [xg[n, i, j].reshape(256, 128) for i in range(4) for j in range(4)]
        squares = jnp.square(cols[0].astype(F32))
        for col in cols[1:]:
            squares = squares + jnp.square(col.astype(F32))
        scale = lax.rsqrt(jnp.sum(squares, axis=1, keepdims=True) / 2048.0 + EPSILON)
        rows = jnp.concatenate(cols, axis=1)
        gate = scale * jnp.dot(rows, wg_v[...], preferred_element_type=F32)
        up = scale * jnp.dot(rows, wu_v[...], preferred_element_type=F32)
        hidden = (gate * (1.0 / (1.0 + jnp.exp(-gate))) * up).astype(BF16)
        for i in range(4):
            block = jnp.dot(hidden, wd_v[:, i * 512:(i + 1) * 512], preferred_element_type=F32).astype(BF16)
            for j in range(4):
                part[n, i, j] = block[:, j * 128:(j + 1) * 128].reshape(8, 32, 128)

    def add(*refs):
        total = refs[0][...].astype(F32)
        for ref in refs[1:]:
            total = total + ref[...].astype(F32)
        return total.astype(BF16)

    own_out = pltpu.make_async_copy(er.at[0, 0], ret.at[ep], own_sem.at[1])

    def scatter_job(n):
        experts(n)
        buf = part.at[n]

        def send(m, src, dst, way):
            return pltpu.make_async_remote_copy(
                src, dst, rs_send.at[m // 8], rs_recv.at[n, m // 4], device_id=near[way], device_id_type=MESH)

        start([
            send(0, buf.at[y2, :, 0:2], r1.at[n, 0], "y+"), send(1, buf.at[y2, :, 2:4], r1.at[n, 1], "y-"),
            send(2, buf.at[:, x2, 4:6], r1.at[n, 2], "x+"), send(3, buf.at[:, x2, 6:8], r1.at[n, 3], "x-")])
        yield
        arrived(buf.at[0], rs_recv.at[n, 0])
        buf[yp, :, 0:2] = add(buf.at[yp, :, 0:2], r1.at[n, 0])
        buf[ym, :, 2:4] = add(buf.at[ym, :, 2:4], r1.at[n, 1])
        buf[:, xp, 4:6] = add(buf.at[:, xp, 4:6], r1.at[n, 2])
        buf[:, xm, 6:8] = add(buf.at[:, xm, 6:8], r1.at[n, 3])
        start([
            send(4, buf.at[yp, :, 0:4], r2.at[n, 0], "y+"), send(5, buf.at[ym, :, 0:4], r2.at[n, 1], "y-"),
            send(6, buf.at[:, xp, 4:8], r2.at[n, 2], "x+"), send(7, buf.at[:, xm, 4:8], r2.at[n, 3], "x-")])
        yield
        arrived(buf.at[0:2], rs_recv.at[n, 1])
        buf[y, :, 0:4] = add(buf.at[y, :, 0:4], r2.at[n, 0], r2.at[n, 1])
        buf[:, x, 4:8] = add(buf.at[:, x, 4:8], r2.at[n, 2], r2.at[n, 3])
        start([
            send(8, buf.at[y, x2, 0:2], r3.at[n, 0], "x+"), send(9, buf.at[y, x2, 2:4], r3.at[n, 1], "x-"),
            send(10, buf.at[y2, x, 4:6], r3.at[n, 2], "y+"), send(11, buf.at[y2, x, 6:8], r3.at[n, 3], "y-")])
        yield
        arrived(buf.at[0, 0], rs_recv.at[n, 2])
        buf[y, xp, 0:2] = add(buf.at[y, xp, 0:2], r3.at[n, 0])
        buf[y, xm, 2:4] = add(buf.at[y, xm, 2:4], r3.at[n, 1])
        buf[yp, x, 4:6] = add(buf.at[yp, x, 4:6], r3.at[n, 2])
        buf[ym, x, 6:8] = add(buf.at[ym, x, 6:8], r3.at[n, 3])
        start([
            send(12, buf.at[y, xp, 0:4], r4.at[n, 0], "x+"), send(13, buf.at[y, xm, 0:4], r4.at[n, 1], "x-"),
            send(14, buf.at[yp, x, 4:8], r4.at[n, 2], "y+"), send(15, buf.at[ym, x, 4:8], r4.at[n, 3], "y-")])
        yield
        arrived(buf.at[0, 0:2], rs_recv.at[n, 3])
        er[n, 0:4] = add(buf.at[y, x, 0:4], r4.at[n, 0], r4.at[n, 1])
        er[n, 4:8] = add(buf.at[y, x, 4:8], r4.at[n, 2], r4.at[n, 3])
        for pos in reversed(range(n * 8, n * 8 + 8)):
            if pos == 0:
                own_out.start()
                continue
            dst = ep_at(OFFS[pos // 2], pos % 2)
            pltpu.make_async_remote_copy(
                er.at[n, pos % 8], ret.at[ep], r_send.at[0], r_recv.at[0],
                device_id=(dst, tp), device_id_type=MESH).start()
        yield

    jobs = {"D": dispatch_job(), "P": proj_job(), "M0": mixer_job(0), "M1": mixer_job(1)}
    for n in range(NCH):
        jobs[f"G{n}"] = gather_job(n)
        jobs[f"S{n}"] = scatter_job(n)
    for item in PLAN:
        next(jobs[item])

    row = lax.broadcasted_iota(jnp.int32, (128, 256), 0)
    w_all = weights[...]
    table = jnp.where(row == 0, p0, 0.0) + jnp.where(row == 1, p1, 0.0)
    table = jnp.where(row == 2, w_all[0:1, :], table)
    table = jnp.where(row == 3, w_all[1:2, :], table)
    cols = table.T
    slot_t = lax.broadcasted_iota(jnp.int32, (256, 1024), 1).astype(F32)
    pick0 = jnp.where(slot_t == cols[:, 0:1], 1.0, 0.0).astype(BF16)
    pick1 = jnp.where(slot_t == cols[:, 1:2], 1.0, 0.0).astype(BF16)
    own_out.wait()
    arrived(ret.at[0:31], r_recv.at[0])
    home = ret[...].reshape(1024, 128)
    out_ref[...] = (cols[:, 2:3] * jnp.dot(pick0, home, preferred_element_type=F32)
                    + cols[:, 3:4] * jnp.dot(pick1, home, preferred_element_type=F32)).astype(BF16)
    halo.wait_send()
    left(disp.at[0:31], d_send.at[0])
    left(ret.at[0:31], r_send.at[0])
    left(xg.at[0, 0:3], ag_send.at[0])
    left(xg.at[0:3], ag_send.at[1])
    left(part.at[0:3], rs_send.at[0])
    left(part.at[0, 0:3], rs_send.at[1])
    left(px.at[0:3], p_send.at[0])
    left(px, p_send.at[1])
    left(px.at[0:3], m_send.at[0])
    left(px.at[0:3], m_send.at[1])


def step(conv_input, out_gate, in_gate, conv_taps, mixer_proj, token_rows, routes, route_weights,
         expert_gate, expert_up, expert_down):
    vmem = pl.BlockSpec(memory_space=pltpu.VMEM)
    hbm = pl.BlockSpec(memory_space=pl.ANY)
    dma = pltpu.SemaphoreType.DMA
    return pl.pallas_call(
        body,
        out_shape=(jax.ShapeDtypeStruct((2048, 128), BF16), jax.ShapeDtypeStruct((256, 128), BF16)),
        in_specs=[hbm, hbm, hbm, vmem, hbm, vmem, vmem, vmem, hbm, hbm, hbm],
        out_specs=(vmem, vmem),
        scratch_shapes=[
            pltpu.VMEM((64, 2048), BF16), pltpu.VMEM((64, 2048), BF16), pltpu.VMEM((64, 2048), BF16),
            pltpu.VMEM((2048, 256), BF16), pltpu.VMEM((2048, 256), BF16), pltpu.VMEM((256, 2048), BF16),
            pltpu.VMEM((64, 2048), BF16), pltpu.VMEM((64, 128), BF16), pltpu.VMEM((1024, 128), F32),
            pltpu.VMEM((4, 1024, 128), BF16), pltpu.VMEM((4, 1024, 128), BF16),
            pltpu.VMEM((4, 4, 64, 128), BF16), pltpu.VMEM((4, 4, 4, 64, 128), BF16),
            pltpu.VMEM((4, 2, 32, 128), BF16), pltpu.VMEM((4, 4, 128, 128), BF16),
            pltpu.VMEM((4, 2, 64, 128), BF16), pltpu.VMEM((4, 4, 128, 128), BF16),
            pltpu.VMEM((32, 32, 128), BF16),
            pltpu.VMEM((NCH, 4, 4, 8, 32, 128), BF16),
            pltpu.VMEM((NCH, 4, 4, 8, 32, 128), BF16),
            pltpu.VMEM((NCH, 8, 32, 128), BF16),
            pltpu.VMEM((32, 32, 128), BF16),
            pltpu.VMEM((NCH, 4, 4, 2, 32, 128), BF16),
            pltpu.VMEM((NCH, 4, 4, 4, 32, 128), BF16),
            pltpu.VMEM((NCH, 4, 2, 32, 128), BF16),
            pltpu.VMEM((NCH, 4, 4, 32, 128), BF16),
            dma((8,)), dma((1,)), dma((NCH,)), dma((1,)), dma((1,)),
            dma((2,)), dma((NCH, 4)), dma((2,)), dma((NCH, 4)), dma((2,)), dma((2, 6)),
            dma((2,)), dma((3,)), dma((2,)), dma((2,)),
        ],
        compiler_params=pltpu.CompilerParams(
            collective_id=0, has_side_effects=True, vmem_limit_bytes=60 * 1024 * 1024),
    )(conv_input, out_gate, in_gate, conv_taps, mixer_proj, token_rows, routes.T, route_weights.T,
      expert_gate, expert_up, expert_down)


def solution(mesh):
    return jax.shard_map(
        step,
        mesh=mesh,
        in_specs=(
            P("tp", "ep"), P("tp", "ep"), P("tp", "ep"), P(), P(None, "tp"), P("ep", "tp"),
            P("ep", None), P("ep", None), P("ep", None, "tp"), P("ep", None, "tp"), P("ep", "tp", None),
        ),
        out_specs=(P("ep", "tp"), P("ep", "tp")),
        check_vma=False,
    )
```
